32 devices in a mesh: sp: 16 (over z, y, x), tp: 2 (over core).
Axes of the slice: x: 2, y: 2, z: 4, core: 2. Of those that a mesh axis runs over, the one named last changes fastest.
Arguments:
- residual: bfloat16 [2048, 2048], P(('sp', 'tp')), may hold values from -24 to 24
- query_small: bfloat16 [2048, 768], P('sp', 'tp'), may hold values from -64 to 64
- query_large: bfloat16 [2048, 1280], P('sp', 'tp'), may hold values from -64 to 64
- latent: bfloat16 [2048, 256], P('sp'), may hold values from -6 to 6
- rope_key: bfloat16 [2048, 32], P('sp'), may hold values from -48 to 48
- key_up_small: bfloat16 [256, 512], P(None, 'tp'), may hold values from -0.375 to 0.375
- value_up_small: bfloat16 [256, 512], P(None, 'tp'), may hold values from -0.375 to 0.375
- key_up_large: bfloat16 [256, 1024], P(None, 'tp'), may hold values from -0.375 to 0.375
- value_up_large: bfloat16 [256, 1024], P(None, 'tp'), may hold values from -0.375 to 0.375
- out_small: bfloat16 [512, 2048], P('tp'), may hold values from -0.625 to 0.625
- out_large: bfloat16 [1024, 2048], P('tp'), may hold values from -0.625 to 0.625
- norm_gain: bfloat16 [2048], replicated, may hold values from 0.099609375 to 1.8984375
- gate_weight: bfloat16 [2048, 5632], P('sp', 'tp'), may hold values from -0.125 to 0.125
- up_weight: bfloat16 [2048, 5632], P('sp', 'tp'), may hold values from -0.125 to 0.125
- down_weight: bfloat16 [2048, 5632], P('sp', 'tp'), may hold values from -0.21875 to 0.21875
Outputs:
- layer_out: bfloat16 [2048, 2048], P(('sp', 'tp'))
The draws below stay inside these ranges and needn't reach their ends.
All inputs are finite; a program needn't handle non-finite values.
Results may differ from the reference program's by a relative error of at most 0.017.
Values may be sent and summed in bfloat16 or wider, within the bound.
A program may use at most 128 MiB of HBM per device.

```python
import jax
import jax.numpy as jnp
from jax import lax

D = 2048
FF = 5632
HEADS_SMALL = 8
HEADS_LARGE = 8
HEAD_SMALL = 64
HEAD_LARGE = 128
ROPE = 32
LATENT = 256
TOKENS = 2048


def draw_residual(key, part):
    subkeys = jax.random.split(key, 3)
    lowest = 0.3
    highest = 3.0
    column = jnp.exp(jax.random.uniform(subkeys[0], (1, D), jnp.float32, jnp.log(lowest), jnp.log(highest)))
    rowscale = jnp.exp(jax.random.uniform(subkeys[1], (TOKENS, 1), jnp.float32, jnp.log(0.5), jnp.log(2.0)))
    sample = jnp.clip(jax.random.normal(subkeys[2], (TOKENS, D), jnp.float32), -4.0, 4.0)
    return jnp.clip(sample * rowscale * column, -24.0, 24.0).astype(jnp.bfloat16)


def drawn_query(key, head_count, head_size):
    span_width = head_size + ROPE
    sample = jnp.clip(2.5 * jax.random.normal(key, (TOKENS, head_count, span_width), jnp.float32), -10.0, 10.0)
    return sample.reshape(TOKENS, head_count * span_width).astype(jnp.bfloat16)


def draw_query_small(key, part):
    return drawn_query(jax.random.fold_in(key, 11), HEADS_SMALL, HEAD_SMALL)


def draw_query_large(key, part):
    return drawn_query(jax.random.fold_in(key, 23), HEADS_LARGE, HEAD_LARGE)


def draw_rope_key(key, part):
    sample = jnp.clip(jax.random.normal(key, (TOKENS, ROPE), jnp.float32), -6.0, 6.0)
    return sample.astype(jnp.bfloat16)


def steps_of(rng, dims, cuts, least, largest):
    def one(position, blocks):
        steps = jax.random.uniform(jax.random.fold_in(jax.random.fold_in(rng, 6), position), (blocks,), jnp.float32, least / len(cuts), largest / len(cuts))
        return jnp.repeat(jnp.exp(steps), dims[position] // blocks).reshape((-1,) + (1,) * (len(dims) - position - 1))

    loudness = one(*cuts[0])
    for cut in cuts[1:]:
        loudness = loudness * one(*cut)
    return loudness


def bell_draw(own_key, shape, spread, reach, shards=(), kind=jnp.bfloat16):
    gain = steps_of(own_key, shape, shards, -0.22, 0.18) if shards else 1.0
    drawn = jax.random.normal(own_key, shape, jnp.float32) * spread * gain
    return jnp.minimum(jnp.maximum(drawn, -reach), reach).astype(kind)


def setup_inputs(seed: int = 0) -> dict:
    seeds = jax.random.split(jax.random.key(seed), 16)
    residual = draw_residual(jax.random.fold_in(seeds[15], 71), 0)
    query_small = draw_query_small(jax.random.fold_in(seeds[15], 71), 0)
    query_large = draw_query_large(jax.random.fold_in(seeds[15], 71), 0)
    latent = bell_draw(seeds[3], (TOKENS, LATENT), 1.0, 6.0, ((0, 16),))
    rope_key = draw_rope_key(jax.random.fold_in(seeds[15], 71), 0)
    key_up_small = bell_draw(seeds[5], (LATENT, HEADS_SMALL * HEAD_SMALL), LATENT ** -0.5, 0.375, ((1, 2),))
    value_up_small = bell_draw(seeds[6], (LATENT, HEADS_SMALL * HEAD_SMALL), LATENT ** -0.5, 0.375, ((1, 2),))
    key_up_large = bell_draw(seeds[7], (LATENT, HEADS_LARGE * HEAD_LARGE), LATENT ** -0.5, 0.375, ((1, 2),))
    value_up_large = bell_draw(seeds[8], (LATENT, HEADS_LARGE * HEAD_LARGE), LATENT ** -0.5, 0.375, ((1, 2),))
    out_small = bell_draw(seeds[9], (HEADS_SMALL * HEAD_SMALL, D), ((HEADS_SMALL * HEAD_SMALL + HEADS_LARGE * HEAD_LARGE) // 16) ** -0.5, 0.625, ((0, 2),))
    out_large = bell_draw(seeds[10], (HEADS_LARGE * HEAD_LARGE, D), ((HEADS_SMALL * HEAD_SMALL + HEADS_LARGE * HEAD_LARGE) // 16) ** -0.5, 0.625, ((0, 2),))
    norm_gain = jnp.clip(1.0 + 0.18 * jax.random.normal(seeds[11], (D,), jnp.float32), 0.099609375, 1.8984375).astype(jnp.bfloat16)
    gate_weight = bell_draw(seeds[12], (D, FF), D ** -0.5, 0.125, ((0, 16), (1, 2)))
    up_weight = bell_draw(seeds[13], (D, FF), D ** -0.5, 0.125, ((0, 16), (1, 2)))
    down_weight = bell_draw(seeds[14], (D, FF), (FF // 8) ** -0.5, 0.21875, ((0, 16), (1, 2)))
    return {"residual": residual, "query_small": query_small, "query_large": query_large, "latent": latent, "rope_key": rope_key, "key_up_small": key_up_small, "value_up_small": value_up_small, "key_up_large": key_up_large, "value_up_large": value_up_large, "out_small": out_small, "out_large": out_large, "norm_gain": norm_gain, "gate_weight": gate_weight, "up_weight": up_weight, "down_weight": down_weight}


big_negative = -1e+30
rope_base = 500000.0
norm_eps = 1e-06

def stored(tensor):
    return lax.optimization_barrier(tensor.astype(jnp.bfloat16))

def rotate_stored(vectors, positions):
    span_width = vectors.shape[-1]
    half_width = span_width // 2
    inverse = 1.0 / rope_base ** (jnp.arange(0, span_width, 2, dtype=jnp.float32) / span_width)
    angles = positions.astype(jnp.float32)[:, None] * inverse[None, :]
    angle_shape = (vectors.shape[0],) + (1,) * (vectors.ndim - 2) + (half_width,)
    cosine = jnp.cos(angles).reshape(angle_shape)
    sine_table = jnp.sin(angles).reshape(angle_shape)
    leading = vectors[..., :half_width].astype(jnp.float32)
    trailing = vectors[..., half_width:].astype(jnp.float32)
    turned = jnp.concatenate([leading * cosine - trailing * sine_table, trailing * cosine + leading * sine_table], axis=-1)
    return stored(turned)

def attend_group(query, latent, key_up, value_up, turned_key, positions, head_count, head_size):
    shaped = query.reshape(TOKENS, head_count, head_size + ROPE)
    nope_part = shaped[..., :head_size]
    turned_query = rotate_stored(shaped[..., head_size:], positions)
    key_rows = stored(jnp.dot(latent, key_up, preferred_element_type=jnp.float32)).reshape(TOKENS, head_count, head_size)
    value_rows = stored(jnp.dot(latent, value_up, preferred_element_type=jnp.float32)).reshape(TOKENS, head_count, head_size)
    scale = (head_size + ROPE) ** (-0.5)
    block_rows = min(256, TOKENS)

    def one_block(block_index):
        offset = block_index * block_rows
        query_nope = lax.dynamic_slice_in_dim(nope_part, offset, block_rows, 0).astype(jnp.float32)
        query_turn = lax.dynamic_slice_in_dim(turned_query, offset, block_rows, 0).astype(jnp.float32)
        query_pos = offset + jnp.arange(block_rows, dtype=jnp.int32)
        scores = jnp.einsum('qhe,khe->qhk', query_nope, key_rows.astype(jnp.float32))
        scores = scores + jnp.einsum('qhr,kr->qhk', query_turn, turned_key.astype(jnp.float32))
        scores = scores * scale
        visible = positions[None, None, :] <= query_pos[:, None, None]
        masked = jnp.where(visible, scores, big_negative)
        maxima = lax.optimization_barrier(jnp.max(masked, axis=2, keepdims=True))
        weights = jnp.where(visible, jnp.exp(masked - maxima), 0.0)
        totals = lax.optimization_barrier(jnp.sum(weights, axis=2))
        rounded = stored(weights).astype(jnp.float32)
        result = jnp.einsum('qhk,khe->qhe', rounded, value_rows.astype(jnp.float32)) / totals[:, :, None]
        return result.reshape(block_rows, head_count * head_size).astype(jnp.bfloat16)
    blocks = lax.map(one_block, jnp.arange(TOKENS // block_rows, dtype=jnp.int32))
    return blocks.reshape(TOKENS, head_count * head_size)

def reference(residual, query_small, query_large, latent, rope_key, key_up_small, value_up_small, key_up_large, value_up_large, out_small, out_large, norm_gain, gate_weight, up_weight, down_weight):
    positions = jnp.arange(TOKENS, dtype=jnp.int32)
    turned_key = rotate_stored(rope_key, positions)
    attended_small = attend_group(query_small, latent, key_up_small, value_up_small, turned_key, positions, HEADS_SMALL, HEAD_SMALL)
    attended_large = attend_group(query_large, latent, key_up_large, value_up_large, turned_key, positions, HEADS_LARGE, HEAD_LARGE)
    mixed = jnp.dot(attended_small, out_small, preferred_element_type=jnp.float32)
    mixed = mixed + jnp.dot(attended_large, out_large, preferred_element_type=jnp.float32)
    mixed = stored(mixed)
    stream = stored(residual.astype(jnp.float32) + mixed.astype(jnp.float32))
    as_float = stream.astype(jnp.float32)
    normed = as_float * lax.rsqrt(lax.optimization_barrier(jnp.mean(as_float * as_float, axis=-1, keepdims=True)) + norm_eps)
    normed = (normed * norm_gain.astype(jnp.float32)[None, :]).astype(jnp.bfloat16)
    gate = jnp.dot(normed, gate_weight, preferred_element_type=jnp.float32)
    up_part = jnp.dot(normed, up_weight, preferred_element_type=jnp.float32)
    hidden = (jax.nn.silu(gate) * up_part).astype(jnp.bfloat16)
    channel = lax.dot_general(hidden, down_weight, (((1,), (1,)), ((), ())), preferred_element_type=jnp.float32)
    channel = stored(channel)
    return (as_float + 0.5 * channel.astype(jnp.float32)).astype(jnp.bfloat16)
```

```python
import jax
import jax.numpy as jnp
from jax import lax
from jax.sharding import PartitionSpec as P

HEAD_SMALL = 64
HEAD_LARGE = 128
ROPE = 32


big_negative = -1e30
rope_base = 500000.0
norm_eps = 1e-06


def rotate(vectors, positions):
    span_width = vectors.shape[-1]
    half_width = span_width // 2
    inverse = 1.0 / rope_base ** (jnp.arange(0, span_width, 2, dtype=jnp.float32) / span_width)
    angles = positions.astype(jnp.float32)[:, None] * inverse[None, :]
    angle_shape = (vectors.shape[0],) + (1,) * (vectors.ndim - 2) + (half_width,)
    cosine = jnp.cos(angles).reshape(angle_shape)
    sine_table = jnp.sin(angles).reshape(angle_shape)
    leading = vectors[..., :half_width].astype(jnp.float32)
    trailing = vectors[..., half_width:].astype(jnp.float32)
    turned = jnp.concatenate(
        [leading * cosine - trailing * sine_table, trailing * cosine + leading * sine_table],
        axis=-1,
    )
    return turned.astype(jnp.bfloat16)


def attend(nope_part, turned_query, key_rows, value_rows, turned_key, visible, head_size):
    head_count, row_count = nope_part.shape[:2]
    key_count = key_rows.shape[0]
    key_rows = key_rows.reshape(key_count, head_count, head_size)
    value_rows = value_rows.reshape(key_count, head_count, head_size)
    scores = jnp.einsum("hqe,khe->hqk", nope_part, key_rows, preferred_element_type=jnp.float32)
    scores = scores + jnp.einsum(
        "hqr,kr->hqk", turned_query, turned_key, preferred_element_type=jnp.float32
    )
    scores = scores * (head_size + ROPE) ** (-0.5)
    masked = jnp.where(visible[None, :, :], scores, big_negative)
    maxima = jnp.max(masked, axis=2)
    weights = jnp.where(visible[None, :, :], jnp.exp(masked - maxima[:, :, None]), 0.0)
    totals = jnp.sum(weights, axis=2)
    summed = jnp.einsum(
        "hqk,khe->hqe", weights.astype(jnp.bfloat16), value_rows, preferred_element_type=jnp.float32
    )
    result = summed / totals[:, :, None]
    return (
        jnp.transpose(result, (1, 0, 2))
        .reshape(row_count, head_count * head_size)
        .astype(jnp.bfloat16)
    )


def shards(
    residual,
    query_small,
    query_large,
    latent,
    rope_key,
    key_up_small,
    value_up_small,
    key_up_large,
    value_up_large,
    out_small,
    out_large,
    norm_gain,
    gate_weight,
    up_weight,
    down_weight,
):
    row_count = query_small.shape[0]
    sp_count = lax.axis_size("sp")
    tp_count = lax.axis_size("tp")
    far = 1
    while far * far < sp_count:
        far *= 2
    near = sp_count // far
    sp_index = lax.axis_index("sp")
    tp_index = lax.axis_index("tp")
    far_index = sp_index // near

    def far_swap(array, step):
        if step == 0:
            return array
        return lax.ppermute(array, "sp", [(i, i ^ (step * near)) for i in range(sp_count)])

    def tp_swap(array, step):
        if step == 0:
            return array
        return lax.ppermute(array, "tp", [(i, i ^ step) for i in range(tp_count)])

    def by_distance(pieces):
        bit = 1
        while bit < far:
            flipped = (far_index & bit) != 0
            pieces = [
                jnp.where(flipped, pieces[place ^ bit], pieces[place]) for place in range(far)
            ]
            bit *= 2
        return pieces

    first_row = sp_index * row_count
    query_pos = first_row + jnp.arange(row_count, dtype=jnp.int32)
    heads_small = key_up_small.shape[1] // HEAD_SMALL
    heads_large = key_up_large.shape[1] // HEAD_LARGE
    latent_width = latent.shape[1]

    own_keys = jnp.concatenate([latent, rotate(rope_key, query_pos)], axis=1)
    all_keys = lax.all_gather(own_keys, "sp", axis=0, tiled=True)

    depth, units = gate_weight.shape
    share = units // far

    def cut(weight):
        return jnp.transpose(weight.reshape(depth, far, share), (1, 0, 2))

    paired = jnp.concatenate([cut(gate_weight), cut(up_weight)], axis=2)
    lowered = cut(down_weight)
    paired_parts = []
    lowered_parts = []
    for step in range(far):
        paired_parts.append(
            far_swap(lax.dynamic_index_in_dim(paired, far_index ^ step, 0, False), step)
        )
    for step in range(far):
        lowered_parts.append(
            far_swap(lax.dynamic_index_in_dim(lowered, far_index ^ step, 0, False), step)
        )
    groups = [[g * near + p for p in range(near)] for g in range(far)]

    def near_gather(array):
        return lax.all_gather(array, "sp", axis=0, tiled=True, axis_index_groups=groups)

    paired_full = [near_gather(part) for part in paired_parts]
    lowered_full = [
        near_gather(jnp.concatenate(lowered_parts[first : first + 2], axis=0))
        for first in range(0, far, 2)
    ]

    def split_query(query, head_count, head_size):
        shaped = query.reshape(row_count, head_count, head_size + ROPE)
        nope_part = jnp.transpose(shaped[..., :head_size], (1, 0, 2))
        turned = jnp.transpose(rotate(shaped[..., head_size:], query_pos), (1, 0, 2))
        return (nope_part, turned)

    nope_small, turned_small = split_query(query_small, heads_small, HEAD_SMALL)
    nope_large, turned_large = split_query(query_large, heads_large, HEAD_LARGE)

    part_latent = all_keys[:, :latent_width]
    turned_key = all_keys[:, latent_width:]
    key_pos = jnp.arange(part_latent.shape[0], dtype=jnp.int32)
    visible = key_pos[None, :] <= query_pos[:, None]

    def lift(weight):
        return jnp.dot(part_latent, weight, preferred_element_type=jnp.float32).astype(
            jnp.bfloat16
        )

    attended_small = attend(
        nope_small,
        turned_small,
        lift(key_up_small),
        lift(value_up_small),
        turned_key,
        visible,
        HEAD_SMALL,
    )
    attended_large = attend(
        nope_large,
        turned_large,
        lift(key_up_large),
        lift(value_up_large),
        turned_key,
        visible,
        HEAD_LARGE,
    )
    share_mixed = jnp.dot(
        attended_small, out_small, preferred_element_type=jnp.float32
    ) + jnp.dot(attended_large, out_large, preferred_element_type=jnp.float32)
    own_rows = row_count // tp_count
    share_mixed = share_mixed.reshape(tp_count, own_rows, share_mixed.shape[1])
    mixed = lax.dynamic_index_in_dim(share_mixed, tp_index, 0, False)
    for step in range(1, tp_count):
        sent = lax.dynamic_index_in_dim(share_mixed, tp_index ^ step, 0, False)
        mixed = mixed + tp_swap(sent.astype(jnp.bfloat16), step).astype(jnp.float32)
    mixed = mixed.astype(jnp.bfloat16)
    stream = (residual.astype(jnp.float32) + mixed.astype(jnp.float32)).astype(jnp.bfloat16)
    as_float = stream.astype(jnp.float32)
    normed = as_float * lax.rsqrt(jnp.mean(as_float * as_float, axis=-1, keepdims=True) + norm_eps)
    normed = (normed * norm_gain.astype(jnp.float32)[None, :]).astype(jnp.bfloat16)

    over_far = jnp.concatenate([far_swap(normed, step) for step in range(far)], axis=0)
    piece = jnp.concatenate([tp_swap(over_far, step) for step in range(tp_count)], axis=0)
    wide = near * depth
    columns = by_distance([piece[:, z * wide : (z + 1) * wide] for z in range(far)])
    both = None
    for step in range(far):
        product = jnp.dot(columns[step], paired_full[step], preferred_element_type=jnp.float32)
        both = product if both is None else both + product
    hidden = (jax.nn.silu(both[:, :share]) * both[:, share:]).astype(jnp.bfloat16)
    blocks = []
    for weight in lowered_full:
        product = lax.dot_general(
            hidden, weight, (((1,), (1,)), ((), ())), preferred_element_type=jnp.float32
        ).astype(jnp.bfloat16)
        product = product.reshape(product.shape[0], near, -1, depth)
        for place in range(product.shape[2]):
            blocks.append(product[:, :, place].reshape(product.shape[0], wide))
    partial = jnp.concatenate(by_distance(blocks), axis=1)
    over_tp = partial.reshape(tp_count, far * own_rows, partial.shape[1])
    summed = over_tp[0].astype(jnp.float32)
    for step in range(1, tp_count):
        summed = summed + tp_swap(over_tp[step], step).astype(jnp.float32)
    summed = summed.astype(jnp.bfloat16).reshape(far, own_rows, partial.shape[1])
    channel = summed[0].astype(jnp.float32)
    for step in range(1, far):
        channel = channel + far_swap(summed[step], step).astype(jnp.float32)
    channel = channel.astype(jnp.bfloat16)
    return (as_float + 0.5 * channel.astype(jnp.float32)).astype(jnp.bfloat16)


def solution(mesh):
    placed = (
        P(("sp", "tp"), None),
        P("sp", "tp"),
        P("sp", "tp"),
        P("sp", None),
        P("sp", None),
        P(None, "tp"),
        P(None, "tp"),
        P(None, "tp"),
        P(None, "tp"),
        P("tp", None),
        P("tp", None),
        P(),
        P("sp", "tp"),
        P("sp", "tp"),
        P("sp", "tp"),
    )
    return jax.shard_map(
        shards, mesh=mesh, in_specs=placed, out_specs=P(("sp", "tp"), None), check_vma=False
    )
```

```python
import jax
import jax.numpy as jnp
from jax import lax
from jax.sharding import PartitionSpec as P

HEAD_SMALL = 64
HEAD_LARGE = 128
ROPE = 32


big_negative = -1e30
rope_base = 500000.0
norm_eps = 1e-06


def rotate(vectors, positions):
    span_width = vectors.shape[-1]
    half_width = span_width // 2
    inverse = 1.0 / rope_base ** (jnp.arange(0, span_width, 2, dtype=jnp.float32) / span_width)
    angles = positions.astype(jnp.float32)[:, None] * inverse[None, :]
    angle_shape = (vectors.shape[0],) + (1,) * (vectors.ndim - 2) + (half_width,)
    cosine = jnp.cos(angles).reshape(angle_shape)
    sine_table = jnp.sin(angles).reshape(angle_shape)
    leading = vectors[..., :half_width].astype(jnp.float32)
    trailing = vectors[..., half_width:].astype(jnp.float32)
    turned = jnp.concatenate(
        [leading * cosine - trailing * sine_table, trailing * cosine + leading * sine_table],
        axis=-1,
    )
    return turned.astype(jnp.bfloat16)


def attend(nope_part, turned_query, key_rows, value_rows, turned_key, visible, head_size):
    head_count, row_count = nope_part.shape[:2]
    key_count = key_rows.shape[0]
    key_rows = key_rows.reshape(key_count, head_count, head_size)
    value_rows = value_rows.reshape(key_count, head_count, head_size)
    scores = jnp.einsum("hqe,khe->hqk", nope_part, key_rows, preferred_element_type=jnp.float32)
    scores = scores + jnp.einsum(
        "hqr,kr->hqk", turned_query, turned_key, preferred_element_type=jnp.float32
    )
    scores = scores * (head_size + ROPE) ** (-0.5)
    masked = jnp.where(visible[None, :, :], scores, big_negative)
    maxima = jnp.max(masked, axis=2)
    weights = jnp.where(visible[None, :, :], jnp.exp(masked - maxima[:, :, None]), 0.0)
    totals = jnp.sum(weights, axis=2)
    summed = jnp.einsum(
        "hqk,khe->hqe", weights.astype(jnp.bfloat16), value_rows, preferred_element_type=jnp.float32
    )
    result = summed / totals[:, :, None]
    return (
        jnp.transpose(result, (1, 0, 2))
        .reshape(row_count, head_count * head_size)
        .astype(jnp.bfloat16)
    )


def shards(
    residual,
    query_small,
    query_large,
    latent,
    rope_key,
    key_up_small,
    value_up_small,
    key_up_large,
    value_up_large,
    out_small,
    out_large,
    norm_gain,
    gate_weight,
    up_weight,
    down_weight,
):
    row_count = query_small.shape[0]
    sp_count = lax.axis_size("sp")
    tp_count = lax.axis_size("tp")
    far = 1
    while far * far < sp_count:
        far *= 2
    near = sp_count // far
    sp_index = lax.axis_index("sp")
    tp_index = lax.axis_index("tp")
    far_index = sp_index // near

    def sp_swap(array, step):
        return lax.ppermute(array, "sp", [(i, i ^ step) for i in range(sp_count)])

    def far_swap(array, step):
        return array if step == 0 else sp_swap(array, step * near)

    def bits_below(count):
        bits = []
        while 1 << len(bits) < count:
            bits.append(1 << len(bits))
        return bits

    def tp_swap(array, step):
        if step == 0:
            return array
        return lax.ppermute(array, "tp", [(i, i ^ step) for i in range(tp_count)])

    def by_distance(pieces):
        for bit in bits_below(sp_count):
            flipped = (sp_index & bit) != 0
            pieces = [
                jnp.where(flipped, pieces[place ^ bit], pieces[place])
                for place in range(sp_count)
            ]
        return pieces

    first_row = sp_index * row_count
    query_pos = first_row + jnp.arange(row_count, dtype=jnp.int32)
    heads_small = key_up_small.shape[1] // HEAD_SMALL
    heads_large = key_up_large.shape[1] // HEAD_LARGE
    latent_width = latent.shape[1]

    own_rows = row_count // tp_count
    own_keys = jnp.concatenate([latent, rotate(rope_key, query_pos)], axis=1)
    all_keys = lax.dynamic_slice_in_dim(own_keys, tp_index * own_rows, own_rows, 0)
    key_order = [0]
    for bit in reversed(bits_below(sp_count)):
        all_keys = jnp.concatenate([all_keys, sp_swap(all_keys, bit)], axis=0)
        key_order = key_order + [place ^ bit for place in key_order]
    all_keys = jnp.concatenate([tp_swap(all_keys, step) for step in range(tp_count)], axis=0)
    key_pos = jnp.concatenate(
        [
            (sp_index ^ place) * row_count
            + (tp_index ^ step) * own_rows
            + jnp.arange(own_rows, dtype=jnp.int32)
            for step in range(tp_count)
            for place in key_order
        ]
    )

    depth, units = gate_weight.shape
    share = units // far

    def cut(weight):
        return jnp.transpose(weight.reshape(depth, far, share), (1, 0, 2))

    paired = jnp.concatenate([cut(gate_weight), cut(up_weight)], axis=2)
    lowered = cut(down_weight)
    paired_parts = []
    lowered_parts = []
    for step in range(far):
        paired_parts.append(
            far_swap(lax.dynamic_index_in_dim(paired, far_index ^ step, 0, False), step)
        )
    for step in range(far):
        lowered_parts.append(
            far_swap(lax.dynamic_index_in_dim(lowered, far_index ^ step, 0, False), step)
        )

    def spread(parts):
        gathered = []
        for number, first in enumerate(range(0, far, far // 2)):
            held = jnp.concatenate(parts[first : first + far // 2], axis=0)
            order = [step * near for step in range(first, first + far // 2)]
            bits = bits_below(near)
            if number:
                bits = bits[::-1]
            for bit in bits[:-1]:
                held = jnp.concatenate([held, sp_swap(held, bit)], axis=0)
                order = order + [place ^ bit for place in order]
            last = bits[-1]
            gathered.append((order, held))
            gathered.append(([place ^ last for place in order], sp_swap(held, last)))
        return gathered

    paired_full = spread(paired_parts)
    lowered_full = spread(lowered_parts)

    def split_query(query, head_count, head_size):
        shaped = query.reshape(row_count, head_count, head_size + ROPE)
        nope_part = jnp.transpose(shaped[..., :head_size], (1, 0, 2))
        turned = jnp.transpose(rotate(shaped[..., head_size:], query_pos), (1, 0, 2))
        return (nope_part, turned)

    nope_small, turned_small = split_query(query_small, heads_small, HEAD_SMALL)
    nope_large, turned_large = split_query(query_large, heads_large, HEAD_LARGE)

    part_latent = all_keys[:, :latent_width]
    turned_key = all_keys[:, latent_width:]
    visible = key_pos[None, :] <= query_pos[:, None]

    def lift(weight):
        return jnp.dot(part_latent, weight, preferred_element_type=jnp.float32).astype(
            jnp.bfloat16
        )

    attended_small = attend(
        nope_small,
        turned_small,
        lift(key_up_small),
        lift(value_up_small),
        turned_key,
        visible,
        HEAD_SMALL,
    )
    attended_large = attend(
        nope_large,
        turned_large,
        lift(key_up_large),
        lift(value_up_large),
        turned_key,
        visible,
        HEAD_LARGE,
    )
    share_mixed = jnp.dot(
        attended_small, out_small, preferred_element_type=jnp.float32
    ) + jnp.dot(attended_large, out_large, preferred_element_type=jnp.float32)
    share_mixed = share_mixed.reshape(tp_count, own_rows, share_mixed.shape[1])
    mixed = lax.dynamic_index_in_dim(share_mixed, tp_index, 0, False)
    for step in range(1, tp_count):
        sent = lax.dynamic_index_in_dim(share_mixed, tp_index ^ step, 0, False)
        mixed = mixed + tp_swap(sent.astype(jnp.bfloat16), step).astype(jnp.float32)
    mixed = mixed.astype(jnp.bfloat16)
    stream = (residual.astype(jnp.float32) + mixed.astype(jnp.float32)).astype(jnp.bfloat16)
    as_float = stream.astype(jnp.float32)
    normed = as_float * lax.rsqrt(jnp.mean(as_float * as_float, axis=-1, keepdims=True) + norm_eps)
    normed = (normed * norm_gain.astype(jnp.float32)[None, :]).astype(jnp.bfloat16)

    piece = normed
    for bit in reversed(bits_below(far)):
        piece = jnp.concatenate([piece, far_swap(piece, bit)], axis=0)
    piece = jnp.concatenate([tp_swap(piece, step) for step in range(tp_count)], axis=0)
    columns = by_distance([piece[:, z * depth : (z + 1) * depth] for z in range(sp_count)])
    both = None
    for order, weight in paired_full:
        rows = jnp.concatenate([columns[place] for place in order], axis=1)
        product = jnp.dot(rows, weight, preferred_element_type=jnp.float32)
        both = product if both is None else both + product
    hidden = (jax.nn.silu(both[:, :share]) * both[:, share:]).astype(jnp.bfloat16)
    blocks = [None] * sp_count
    for order, weight in lowered_full:
        product = lax.dot_general(
            hidden, weight, (((1,), (1,)), ((), ())), preferred_element_type=jnp.float32
        ).astype(jnp.bfloat16)
        for number, place in enumerate(order):
            blocks[place] = product[:, number * depth : (number + 1) * depth]
    partial = jnp.concatenate(by_distance(blocks), axis=1)
    over_tp = partial.reshape(tp_count, far * own_rows, partial.shape[1])
    summed = over_tp[0].astype(jnp.float32)
    for step in range(1, tp_count):
        summed = summed + tp_swap(over_tp[step], step).astype(jnp.float32)
    for bit in bits_below(far):
        half = summed.shape[0] // 2
        sent = far_swap(summed[half:].astype(jnp.bfloat16), bit)
        summed = summed[:half] + sent.astype(jnp.float32)
    channel = summed
    channel = channel.astype(jnp.bfloat16)
    return (as_float + 0.5 * channel.astype(jnp.float32)).astype(jnp.bfloat16)


def solution(mesh):
    placed = (
        P(("sp", "tp"), None),
        P("sp", "tp"),
        P("sp", "tp"),
        P("sp", None),
        P("sp", None),
        P(None, "tp"),
        P(None, "tp"),
        P(None, "tp"),
        P(None, "tp"),
        P("tp", None),
        P("tp", None),
        P(),
        P("sp", "tp"),
        P("sp", "tp"),
        P("sp", "tp"),
    )
    return jax.shard_map(
        shards, mesh=mesh, in_specs=placed, out_specs=P(("sp", "tp"), None), check_vma=False
    )
```

```python
import jax
import jax.numpy as jnp
from jax import lax
from jax.sharding import PartitionSpec as P

HEAD_SMALL = 64
HEAD_LARGE = 128
ROPE = 32


big_negative = -1e30
rope_base = 500000.0
norm_eps = 1e-06


def rotate(vectors, positions):
    span_width = vectors.shape[-1]
    half_width = span_width // 2
    inverse = 1.0 / rope_base ** (jnp.arange(0, span_width, 2, dtype=jnp.float32) / span_width)
    angles = positions.astype(jnp.float32)[:, None] * inverse[None, :]
    angle_shape = (vectors.shape[0],) + (1,) * (vectors.ndim - 2) + (half_width,)
    cosine = jnp.cos(angles).reshape(angle_shape)
    sine_table = jnp.sin(angles).reshape(angle_shape)
    leading = vectors[..., :half_width].astype(jnp.float32)
    trailing = vectors[..., half_width:].astype(jnp.float32)
    turned = jnp.concatenate(
        [leading * cosine - trailing * sine_table, trailing * cosine + leading * sine_table],
        axis=-1,
    )
    return turned.astype(jnp.bfloat16)


def attend(nope_part, turned_query, key_rows, value_rows, turned_key, visible, head_size):
    head_count, row_count = nope_part.shape[:2]
    key_count = key_rows.shape[0]
    key_rows = key_rows.reshape(key_count, head_count, head_size)
    value_rows = value_rows.reshape(key_count, head_count, head_size)
    scores = jnp.einsum("hqe,khe->hqk", nope_part, key_rows, preferred_element_type=jnp.float32)
    scores = scores + jnp.einsum(
        "hqr,kr->hqk", turned_query, turned_key, preferred_element_type=jnp.float32
    )
    scores = scores * (head_size + ROPE) ** (-0.5)
    masked = jnp.where(visible[None, :, :], scores, big_negative)
    maxima = jnp.max(masked, axis=2)
    weights = jnp.where(visible[None, :, :], jnp.exp(masked - maxima[:, :, None]), 0.0)
    totals = jnp.sum(weights, axis=2)
    summed = jnp.einsum(
        "hqk,khe->hqe", weights.astype(jnp.bfloat16), value_rows, preferred_element_type=jnp.float32
    )
    result = summed / totals[:, :, None]
    return (
        jnp.transpose(result, (1, 0, 2))
        .reshape(row_count, head_count * head_size)
        .astype(jnp.bfloat16)
    )


def shards(
    residual,
    query_small,
    query_large,
    latent,
    rope_key,
    key_up_small,
    value_up_small,
    key_up_large,
    value_up_large,
    out_small,
    out_large,
    norm_gain,
    gate_weight,
    up_weight,
    down_weight,
):
    row_count = query_small.shape[0]
    sp_count = lax.axis_size("sp")
    tp_count = lax.axis_size("tp")
    far = 1
    while far * far < sp_count:
        far *= 2
    near = sp_count // far
    sp_index = lax.axis_index("sp")
    tp_index = lax.axis_index("tp")
    far_index = sp_index // near

    def sp_swap(array, step):
        return lax.ppermute(array, "sp", [(i, i ^ step) for i in range(sp_count)])

    def far_swap(array, step):
        return array if step == 0 else sp_swap(array, step * near)

    def bits_below(count):
        bits = []
        while 1 << len(bits) < count:
            bits.append(1 << len(bits))
        return bits

    def tp_swap(array, step):
        if step == 0:
            return array
        return lax.ppermute(array, "tp", [(i, i ^ step) for i in range(tp_count)])

    def by_distance(pieces):
        for bit in bits_below(sp_count):
            flipped = (sp_index & bit) != 0
            pieces = [
                jnp.where(flipped, pieces[place ^ bit], pieces[place])
                for place in range(sp_count)
            ]
        return pieces

    first_row = sp_index * row_count
    query_pos = first_row + jnp.arange(row_count, dtype=jnp.int32)
    heads_small = key_up_small.shape[1] // HEAD_SMALL
    heads_large = key_up_large.shape[1] // HEAD_LARGE
    latent_width = latent.shape[1]

    own_rows = row_count // tp_count
    own_keys = jnp.concatenate([latent, rotate(rope_key, query_pos)], axis=1)
    all_keys = lax.dynamic_slice_in_dim(own_keys, tp_index * own_rows, own_rows, 0)
    key_order = [0]
    for bit in reversed(bits_below(sp_count)):
        all_keys = jnp.concatenate([all_keys, sp_swap(all_keys, bit)], axis=0)
        key_order = key_order + [place ^ bit for place in key_order]
    all_keys = jnp.concatenate([tp_swap(all_keys, step) for step in range(tp_count)], axis=0)
    key_pos = jnp.concatenate(
        [
            (sp_index ^ place) * row_count
            + (tp_index ^ step) * own_rows
            + jnp.arange(own_rows, dtype=jnp.int32)
            for step in range(tp_count)
            for place in key_order
        ]
    )

    depth, units = gate_weight.shape
    share = units // far

    def cut(weight):
        return jnp.transpose(weight.reshape(depth, far, share), (1, 0, 2))

    paired = jnp.concatenate([cut(gate_weight), cut(up_weight)], axis=2)
    lowered = cut(down_weight)
    paired_parts = []
    lowered_parts = []
    for step in range(far):
        paired_parts.append(
            far_swap(lax.dynamic_index_in_dim(paired, far_index ^ step, 0, False), step)
        )
    for step in range(far):
        lowered_parts.append(
            far_swap(lax.dynamic_index_in_dim(lowered, far_index ^ step, 0, False), step)
        )

    all_keys, paired_parts = lax.optimization_barrier((all_keys, paired_parts))

    def widen(parts):
        halves = []
        for number, first in enumerate(range(0, far, far // 2)):
            held = jnp.concatenate(parts[first : first + far // 2], axis=0)
            order = [step * near for step in range(first, first + far // 2)]
            bits = bits_below(near)
            if number:
                bits = bits[::-1]
            for bit in bits[:-1]:
                held = jnp.concatenate([held, sp_swap(held, bit)], axis=0)
                order = order + [place ^ bit for place in order]
            halves.append((order, bits[-1], held))
        return [(order, bit) for order, bit, _ in halves], [held for _, _, held in halves]

    def complete(plans, halves):
        gathered = []
        for (order, bit), held in zip(plans, halves):
            gathered.append((order, held))
            gathered.append(([place ^ bit for place in order], sp_swap(held, bit)))
        return gathered

    paired_plans, paired_halves = widen(paired_parts)

    def split_query(query, head_count, head_size):
        shaped = query.reshape(row_count, head_count, head_size + ROPE)
        nope_part = jnp.transpose(shaped[..., :head_size], (1, 0, 2))
        turned = jnp.transpose(rotate(shaped[..., head_size:], query_pos), (1, 0, 2))
        return (nope_part, turned)

    nope_small, turned_small = split_query(query_small, heads_small, HEAD_SMALL)
    nope_large, turned_large = split_query(query_large, heads_large, HEAD_LARGE)

    part_latent = all_keys[:, :latent_width]
    turned_key = all_keys[:, latent_width:]
    visible = key_pos[None, :] <= query_pos[:, None]

    def lift(weight):
        return jnp.dot(part_latent, weight, preferred_element_type=jnp.float32).astype(
            jnp.bfloat16
        )

    attended_small = attend(
        nope_small,
        turned_small,
        lift(key_up_small),
        lift(value_up_small),
        turned_key,
        visible,
        HEAD_SMALL,
    )
    attended_small, part_latent, paired_halves, lowered_parts = lax.optimization_barrier(
        (attended_small, part_latent, paired_halves, lowered_parts)
    )
    paired_full = complete(paired_plans, paired_halves)
    lowered_plans, lowered_halves = widen(lowered_parts)
    attended_large = attend(
        nope_large,
        turned_large,
        lift(key_up_large),
        lift(value_up_large),
        turned_key,
        visible,
        HEAD_LARGE,
    )
    share_mixed = jnp.dot(
        attended_small, out_small, preferred_element_type=jnp.float32
    ) + jnp.dot(attended_large, out_large, preferred_element_type=jnp.float32)
    share_mixed = share_mixed.reshape(tp_count, own_rows, share_mixed.shape[1])
    mixed = lax.dynamic_index_in_dim(share_mixed, tp_index, 0, False)
    for step in range(1, tp_count):
        sent = lax.dynamic_index_in_dim(share_mixed, tp_index ^ step, 0, False)
        mixed = mixed + tp_swap(sent.astype(jnp.bfloat16), step).astype(jnp.float32)
    mixed = mixed.astype(jnp.bfloat16)
    stream = (residual.astype(jnp.float32) + mixed.astype(jnp.float32)).astype(jnp.bfloat16)
    as_float = stream.astype(jnp.float32)
    normed = as_float * lax.rsqrt(jnp.mean(as_float * as_float, axis=-1, keepdims=True) + norm_eps)
    normed = (normed * norm_gain.astype(jnp.float32)[None, :]).astype(jnp.bfloat16)

    paired_weights = [weight for _, weight in paired_full]
    normed, paired_weights, lowered_halves = lax.optimization_barrier(
        (normed, paired_weights, lowered_halves)
    )
    lowered_full = complete(lowered_plans, lowered_halves)
    piece = normed
    for bit in reversed(bits_below(far)):
        piece = jnp.concatenate([piece, far_swap(piece, bit)], axis=0)
    piece = jnp.concatenate([tp_swap(piece, step) for step in range(tp_count)], axis=0)
    columns = by_distance([piece[:, z * depth : (z + 1) * depth] for z in range(sp_count)])
    both = None
    for (order, _), weight in zip(paired_full, paired_weights):
        rows = jnp.concatenate([columns[place] for place in order], axis=1)
        product = jnp.dot(rows, weight, preferred_element_type=jnp.float32)
        both = product if both is None else both + product
    hidden = (jax.nn.silu(both[:, :share]) * both[:, share:]).astype(jnp.bfloat16)
    blocks = [None] * sp_count
    for order, weight in lowered_full:
        product = lax.dot_general(
            hidden, weight, (((1,), (1,)), ((), ())), preferred_element_type=jnp.float32
        ).astype(jnp.bfloat16)
        for number, place in enumerate(order):
            blocks[place] = product[:, number * depth : (number + 1) * depth]
    partial = jnp.concatenate(by_distance(blocks), axis=1)
    over_tp = partial.reshape(tp_count, far * own_rows, partial.shape[1])
    summed = over_tp[0].astype(jnp.float32)
    for step in range(1, tp_count):
        summed = summed + tp_swap(over_tp[step], step).astype(jnp.float32)
    for bit in bits_below(far):
        half = summed.shape[0] // 2
        sent = far_swap(summed[half:].astype(jnp.bfloat16), bit)
        summed = summed[:half] + sent.astype(jnp.float32)
    channel = summed
    channel = channel.astype(jnp.bfloat16)
    return (as_float + 0.5 * channel.astype(jnp.float32)).astype(jnp.bfloat16)


def solution(mesh):
    placed = (
        P(("sp", "tp"), None),
        P("sp", "tp"),
        P("sp", "tp"),
        P("sp", None),
        P("sp", None),
        P(None, "tp"),
        P(None, "tp"),
        P(None, "tp"),
        P(None, "tp"),
        P("tp", None),
        P("tp", None),
        P(),
        P("sp", "tp"),
        P("sp", "tp"),
        P("sp", "tp"),
    )
    return jax.shard_map(
        shards, mesh=mesh, in_specs=placed, out_specs=P(("sp", "tp"), None), check_vma=False
    )
```

```python
import jax
import jax.numpy as jnp
from jax import lax
from jax.sharding import PartitionSpec as P

HEAD_SMALL = 64
HEAD_LARGE = 128
ROPE = 32


big_negative = -1e30
rope_base = 500000.0
norm_eps = 1e-06


def rotate(vectors, positions):
    span_width = vectors.shape[-1]
    half_width = span_width // 2
    inverse = 1.0 / rope_base ** (jnp.arange(0, span_width, 2, dtype=jnp.float32) / span_width)
    angles = positions.astype(jnp.float32)[:, None] * inverse[None, :]
    angle_shape = (vectors.shape[0],) + (1,) * (vectors.ndim - 2) + (half_width,)
    cosine = jnp.cos(angles).reshape(angle_shape)
    sine_table = jnp.sin(angles).reshape(angle_shape)
    leading = vectors[..., :half_width].astype(jnp.float32)
    trailing = vectors[..., half_width:].astype(jnp.float32)
    turned = jnp.concatenate(
        [leading * cosine - trailing * sine_table, trailing * cosine + leading * sine_table],
        axis=-1,
    )
    return turned.astype(jnp.bfloat16)


def attend(nope_part, turned_query, key_rows, value_rows, turned_key, visible, head_size):
    head_count, row_count = nope_part.shape[:2]
    key_count = key_rows.shape[0]
    key_rows = key_rows.reshape(key_count, head_count, head_size)
    value_rows = value_rows.reshape(key_count, head_count, head_size)
    scores = jnp.einsum("hqe,khe->hqk", nope_part, key_rows, preferred_element_type=jnp.float32)
    scores = scores + jnp.einsum(
        "hqr,kr->hqk", turned_query, turned_key, preferred_element_type=jnp.float32
    )
    scores = scores * (head_size + ROPE) ** (-0.5)
    masked = jnp.where(visible[None, :, :], scores, big_negative)
    maxima = jnp.max(masked, axis=2)
    weights = jnp.where(visible[None, :, :], jnp.exp(masked - maxima[:, :, None]), 0.0)
    totals = jnp.sum(weights, axis=2)
    summed = jnp.einsum(
        "hqk,khe->hqe", weights.astype(jnp.bfloat16), value_rows, preferred_element_type=jnp.float32
    )
    result = summed / totals[:, :, None]
    return (
        jnp.transpose(result, (1, 0, 2))
        .reshape(row_count, head_count * head_size)
        .astype(jnp.bfloat16)
    )


def shards(
    residual,
    query_small,
    query_large,
    latent,
    rope_key,
    key_up_small,
    value_up_small,
    key_up_large,
    value_up_large,
    out_small,
    out_large,
    norm_gain,
    gate_weight,
    up_weight,
    down_weight,
):
    row_count = query_small.shape[0]
    sp_count = lax.axis_size("sp")
    tp_count = lax.axis_size("tp")
    far = 1
    while far * far < sp_count:
        far *= 2
    near = sp_count // far
    sp_index = lax.axis_index("sp")
    tp_index = lax.axis_index("tp")
    far_index = sp_index // near

    def sp_swap(array, step):
        return lax.ppermute(array, "sp", [(i, i ^ step) for i in range(sp_count)])

    def far_swap(array, step):
        return array if step == 0 else sp_swap(array, step * near)

    def bits_below(count):
        bits = []
        while 1 << len(bits) < count:
            bits.append(1 << len(bits))
        return bits

    def tp_swap(array, step):
        if step == 0:
            return array
        return lax.ppermute(array, "tp", [(i, i ^ step) for i in range(tp_count)])

    def by_distance(pieces):
        for bit in bits_below(sp_count):
            flipped = (sp_index & bit) != 0
            pieces = [
                jnp.where(flipped, pieces[place ^ bit], pieces[place])
                for place in range(sp_count)
            ]
        return pieces

    first_row = sp_index * row_count
    query_pos = first_row + jnp.arange(row_count, dtype=jnp.int32)
    heads_small = key_up_small.shape[1] // HEAD_SMALL
    heads_large = key_up_large.shape[1] // HEAD_LARGE
    latent_width = latent.shape[1]

    own_rows = row_count // tp_count
    own_keys = jnp.concatenate([latent, rotate(rope_key, query_pos)], axis=1)
    all_keys = lax.dynamic_slice_in_dim(own_keys, tp_index * own_rows, own_rows, 0)
    key_order = [0]
    for bit in reversed(bits_below(sp_count)):
        all_keys = jnp.concatenate([all_keys, sp_swap(all_keys, bit)], axis=0)
        key_order = key_order + [place ^ bit for place in key_order]
    all_keys = jnp.concatenate([tp_swap(all_keys, step) for step in range(tp_count)], axis=0)
    key_pos = jnp.concatenate(
        [
            (sp_index ^ place) * row_count
            + (tp_index ^ step) * own_rows
            + jnp.arange(own_rows, dtype=jnp.int32)
            for step in range(tp_count)
            for place in key_order
        ]
    )

    depth, units = gate_weight.shape
    share = units // far

    def cut(weight):
        return jnp.transpose(weight.reshape(depth, far, share), (1, 0, 2))

    paired = jnp.concatenate([cut(gate_weight), cut(up_weight)], axis=2)
    lowered = cut(down_weight)
    paired_parts = []
    lowered_parts = []
    for step in range(far):
        paired_parts.append(
            far_swap(lax.dynamic_index_in_dim(paired, far_index ^ step, 0, False), step)
        )
    for step in range(far):
        lowered_parts.append(
            far_swap(lax.dynamic_index_in_dim(lowered, far_index ^ step, 0, False), step)
        )

    all_keys, paired_parts = lax.optimization_barrier((all_keys, paired_parts))

    def widen(parts):
        plans = []
        early = []
        late = []
        for number, first in enumerate(range(0, far, far // 2)):
            held = jnp.concatenate(parts[first : first + far // 2], axis=0)
            order = [step * near for step in range(first, first + far // 2)]
            bits = bits_below(near)
            if number:
                bits = bits[::-1]
            for bit in bits[:-2]:
                held = jnp.concatenate([held, sp_swap(held, bit)], axis=0)
                order = order + [place ^ bit for place in order]
            plans.append((order, bits[-2], bits[-1]))
            early.append(held)
            late.append(sp_swap(held, bits[-2]))
        return plans, early, late

    def across(plans, blocks):
        return [sp_swap(block, last) for (_, _, last), block in zip(plans, blocks)]

    def orders_of(plans):
        orders = []
        for order, bit, last in plans:
            turned = [place ^ bit for place in order]
            orders.append(order)
            orders.append(turned)
            orders.append([place ^ last for place in order])
            orders.append([place ^ last for place in turned])
        return orders

    paired_plans, paired_early, paired_late = widen(paired_parts)

    def split_query(query, head_count, head_size):
        shaped = query.reshape(row_count, head_count, head_size + ROPE)
        nope_part = jnp.transpose(shaped[..., :head_size], (1, 0, 2))
        turned = jnp.transpose(rotate(shaped[..., head_size:], query_pos), (1, 0, 2))
        return (nope_part, turned)

    nope_small, turned_small = split_query(query_small, heads_small, HEAD_SMALL)
    nope_large, turned_large = split_query(query_large, heads_large, HEAD_LARGE)

    part_latent = all_keys[:, :latent_width]
    turned_key = all_keys[:, latent_width:]
    visible = key_pos[None, :] <= query_pos[:, None]

    def lift(weight):
        return jnp.dot(part_latent, weight, preferred_element_type=jnp.float32).astype(
            jnp.bfloat16
        )

    attended_small = attend(
        nope_small,
        turned_small,
        lift(key_up_small),
        lift(value_up_small),
        turned_key,
        visible,
        HEAD_SMALL,
    )
    attended_small, part_latent, paired_early, paired_late, lowered_parts = (
        lax.optimization_barrier(
            (attended_small, part_latent, paired_early, paired_late, lowered_parts)
        )
    )
    paired_near = across(paired_plans, paired_early)
    lowered_plans, lowered_early, lowered_late = widen(lowered_parts)
    attended_large = attend(
        nope_large,
        turned_large,
        lift(key_up_large),
        lift(value_up_large),
        turned_key,
        visible,
        HEAD_LARGE,
    )
    attended_large, paired_near, paired_late = lax.optimization_barrier(
        (attended_large, paired_near, paired_late)
    )
    paired_far = across(paired_plans, paired_late)
    share_mixed = jnp.dot(
        attended_small, out_small, preferred_element_type=jnp.float32
    ) + jnp.dot(attended_large, out_large, preferred_element_type=jnp.float32)
    share_mixed = share_mixed.reshape(tp_count, own_rows, share_mixed.shape[1])
    mixed = lax.dynamic_index_in_dim(share_mixed, tp_index, 0, False)
    for step in range(1, tp_count):
        sent = lax.dynamic_index_in_dim(share_mixed, tp_index ^ step, 0, False)
        mixed = mixed + tp_swap(sent.astype(jnp.bfloat16), step).astype(jnp.float32)
    mixed = mixed.astype(jnp.bfloat16)
    stream = (residual.astype(jnp.float32) + mixed.astype(jnp.float32)).astype(jnp.bfloat16)
    as_float = stream.astype(jnp.float32)
    normed = as_float * lax.rsqrt(jnp.mean(as_float * as_float, axis=-1, keepdims=True) + norm_eps)
    normed = (normed * norm_gain.astype(jnp.float32)[None, :]).astype(jnp.bfloat16)

    piece = normed
    for number, bit in enumerate(reversed(bits_below(far))):
        if number == 1:
            piece, paired_far, lowered_early, lowered_late = lax.optimization_barrier(
                (piece, paired_far, lowered_early, lowered_late)
            )
        piece = jnp.concatenate([piece, far_swap(piece, bit)], axis=0)
    lowered_near = across(lowered_plans, lowered_early)
    lowered_far = across(lowered_plans, lowered_late)

    def in_order(*kinds):
        return [block for group in zip(*kinds) for block in group]

    paired_weights = in_order(paired_early, paired_late, paired_near, paired_far)
    lowered_weights = in_order(lowered_early, lowered_late, lowered_near, lowered_far)
    piece = jnp.concatenate([tp_swap(piece, step) for step in range(tp_count)], axis=0)
    columns = by_distance([piece[:, z * depth : (z + 1) * depth] for z in range(sp_count)])
    both = None
    for order, weight in zip(orders_of(paired_plans), paired_weights):
        rows = jnp.concatenate([columns[place] for place in order], axis=1)
        product = jnp.dot(rows, weight, preferred_element_type=jnp.float32)
        both = product if both is None else both + product
    hidden = (jax.nn.silu(both[:, :share]) * both[:, share:]).astype(jnp.bfloat16)
    blocks = [None] * sp_count
    for order, weight in zip(orders_of(lowered_plans), lowered_weights):
        product = lax.dot_general(
            hidden, weight, (((1,), (1,)), ((), ())), preferred_element_type=jnp.float32
        ).astype(jnp.bfloat16)
        for number, place in enumerate(order):
            blocks[place] = product[:, number * depth : (number + 1) * depth]
    partial = jnp.concatenate(by_distance(blocks), axis=1)
    over_tp = partial.reshape(tp_count, far * own_rows, partial.shape[1])
    summed = over_tp[0].astype(jnp.float32)
    for step in range(1, tp_count):
        summed = summed + tp_swap(over_tp[step], step).astype(jnp.float32)
    for bit in bits_below(far):
        half = summed.shape[0] // 2
        sent = far_swap(summed[half:].astype(jnp.bfloat16), bit)
        summed = summed[:half] + sent.astype(jnp.float32)
    channel = summed
    channel = channel.astype(jnp.bfloat16)
    return (as_float + 0.5 * channel.astype(jnp.float32)).astype(jnp.bfloat16)


def solution(mesh):
    placed = (
        P(("sp", "tp"), None),
        P("sp", "tp"),
        P("sp", "tp"),
        P("sp", None),
        P("sp", None),
        P(None, "tp"),
        P(None, "tp"),
        P(None, "tp"),
        P(None, "tp"),
        P("tp", None),
        P("tp", None),
        P(),
        P("sp", "tp"),
        P("sp", "tp"),
        P("sp", "tp"),
    )
    return jax.shard_map(
        shards, mesh=mesh, in_specs=placed, out_specs=P(("sp", "tp"), None), check_vma=False
    )
```

```python
import jax
import jax.numpy as jnp
from jax import lax
from jax.sharding import PartitionSpec as P

HEAD_SMALL = 64
HEAD_LARGE = 128
ROPE = 32


big_negative = -1e30
rope_base = 500000.0
norm_eps = 1e-06


def rotate(vectors, positions):
    span_width = vectors.shape[-1]
    half_width = span_width // 2
    inverse = 1.0 / rope_base ** (jnp.arange(0, span_width, 2, dtype=jnp.float32) / span_width)
    angles = positions.astype(jnp.float32)[:, None] * inverse[None, :]
    angle_shape = (vectors.shape[0],) + (1,) * (vectors.ndim - 2) + (half_width,)
    cosine = jnp.cos(angles).reshape(angle_shape)
    sine_table = jnp.sin(angles).reshape(angle_shape)
    leading = vectors[..., :half_width].astype(jnp.float32)
    trailing = vectors[..., half_width:].astype(jnp.float32)
    turned = jnp.concatenate(
        [leading * cosine - trailing * sine_table, trailing * cosine + leading * sine_table],
        axis=-1,
    )
    return turned.astype(jnp.bfloat16)


def attend(nope_part, turned_query, key_rows, value_rows, turned_key, visible, head_size):
    head_count, row_count = nope_part.shape[:2]
    key_count = key_rows.shape[0]
    key_rows = key_rows.reshape(key_count, head_count, head_size)
    value_rows = value_rows.reshape(key_count, head_count, head_size)
    scores = jnp.einsum("hqe,khe->hqk", nope_part, key_rows, preferred_element_type=jnp.float32)
    scores = scores + jnp.einsum(
        "hqr,kr->hqk", turned_query, turned_key, preferred_element_type=jnp.float32
    )
    scores = scores * (head_size + ROPE) ** (-0.5)
    masked = jnp.where(visible[None, :, :], scores, big_negative)
    maxima = jnp.max(masked, axis=2)
    weights = jnp.where(visible[None, :, :], jnp.exp(masked - maxima[:, :, None]), 0.0)
    totals = jnp.sum(weights, axis=2)
    summed = jnp.einsum(
        "hqk,khe->hqe", weights.astype(jnp.bfloat16), value_rows, preferred_element_type=jnp.float32
    )
    result = summed / totals[:, :, None]
    return (
        jnp.transpose(result, (1, 0, 2))
        .reshape(row_count, head_count * head_size)
        .astype(jnp.bfloat16)
    )


def shards(
    residual,
    query_small,
    query_large,
    latent,
    rope_key,
    key_up_small,
    value_up_small,
    key_up_large,
    value_up_large,
    out_small,
    out_large,
    norm_gain,
    gate_weight,
    up_weight,
    down_weight,
):
    row_count = query_small.shape[0]
    sp_count = lax.axis_size("sp")
    tp_count = lax.axis_size("tp")
    far = 1
    while far * far < sp_count:
        far *= 2
    near = sp_count // far
    sp_index = lax.axis_index("sp")
    tp_index = lax.axis_index("tp")
    far_index = sp_index // near

    def sp_swap(array, step):
        return lax.ppermute(array, "sp", [(i, i ^ step) for i in range(sp_count)])

    def far_swap(array, step):
        return array if step == 0 else sp_swap(array, step * near)

    def bits_below(count):
        bits = []
        while 1 << len(bits) < count:
            bits.append(1 << len(bits))
        return bits

    def tp_swap(array, step):
        if step == 0:
            return array
        return lax.ppermute(array, "tp", [(i, i ^ step) for i in range(tp_count)])

    def by_distance(pieces):
        for bit in bits_below(sp_count):
            flipped = (sp_index & bit) != 0
            pieces = [
                jnp.where(flipped, pieces[place ^ bit], pieces[place])
                for place in range(sp_count)
            ]
        return pieces

    first_row = sp_index * row_count
    query_pos = first_row + jnp.arange(row_count, dtype=jnp.int32)
    heads_small = key_up_small.shape[1] // HEAD_SMALL
    heads_large = key_up_large.shape[1] // HEAD_LARGE
    latent_width = latent.shape[1]

    own_rows = row_count // tp_count
    depth, units = gate_weight.shape
    share = units // far

    def cut(weight):
        return jnp.transpose(weight.reshape(depth, far, share), (1, 0, 2))

    paired = jnp.concatenate([cut(gate_weight), cut(up_weight)], axis=2)
    lowered = cut(down_weight)
    own_keys = jnp.concatenate([latent, rotate(rope_key, query_pos)], axis=1)
    all_keys = lax.dynamic_slice_in_dim(own_keys, tp_index * own_rows, own_rows, 0)
    key_order = [0]
    for bit in reversed(bits_below(sp_count)):
        all_keys = jnp.concatenate([all_keys, sp_swap(all_keys, bit)], axis=0)
        key_order = key_order + [place ^ bit for place in key_order]
        if bit == near:
            all_keys, paired, lowered = lax.optimization_barrier((all_keys, paired, lowered))
    all_keys = jnp.concatenate([tp_swap(all_keys, step) for step in range(tp_count)], axis=0)
    key_pos = jnp.concatenate(
        [
            (sp_index ^ place) * row_count
            + (tp_index ^ step) * own_rows
            + jnp.arange(own_rows, dtype=jnp.int32)
            for step in range(tp_count)
            for place in key_order
        ]
    )

    paired_parts = []
    lowered_parts = []
    for step in range(far):
        paired_parts.append(
            far_swap(lax.dynamic_index_in_dim(paired, far_index ^ step, 0, False), step)
        )
    for step in range(far):
        lowered_parts.append(
            far_swap(lax.dynamic_index_in_dim(lowered, far_index ^ step, 0, False), step)
        )

    all_keys, paired_parts = lax.optimization_barrier((all_keys, paired_parts))

    def widen(parts):
        plans = []
        early = []
        late = []
        for number, first in enumerate(range(0, far, far // 2)):
            held = jnp.concatenate(parts[first : first + far // 2], axis=0)
            order = [step * near for step in range(first, first + far // 2)]
            bits = bits_below(near)
            if number:
                bits = bits[::-1]
            for bit in bits[:-2]:
                held = jnp.concatenate([held, sp_swap(held, bit)], axis=0)
                order = order + [place ^ bit for place in order]
            plans.append((order, bits[-2], bits[-1]))
            early.append(held)
            late.append(sp_swap(held, bits[-2]))
        return plans, early, late

    def across(plans, blocks):
        return [sp_swap(block, last) for (_, _, last), block in zip(plans, blocks)]

    def orders_of(plans):
        orders = []
        for order, bit, last in plans:
            turned = [place ^ bit for place in order]
            orders.append(order)
            orders.append(turned)
            orders.append([place ^ last for place in order])
            orders.append([place ^ last for place in turned])
        return orders

    paired_plans, paired_early, paired_late = widen(paired_parts)

    def split_query(query, head_count, head_size):
        shaped = query.reshape(row_count, head_count, head_size + ROPE)
        nope_part = jnp.transpose(shaped[..., :head_size], (1, 0, 2))
        turned = jnp.transpose(rotate(shaped[..., head_size:], query_pos), (1, 0, 2))
        return (nope_part, turned)

    nope_small, turned_small = split_query(query_small, heads_small, HEAD_SMALL)
    nope_large, turned_large = split_query(query_large, heads_large, HEAD_LARGE)

    part_latent = all_keys[:, :latent_width]
    turned_key = all_keys[:, latent_width:]
    visible = key_pos[None, :] <= query_pos[:, None]

    def lift(weight):
        return jnp.dot(part_latent, weight, preferred_element_type=jnp.float32).astype(
            jnp.bfloat16
        )

    attended_small = attend(
        nope_small,
        turned_small,
        lift(key_up_small),
        lift(value_up_small),
        turned_key,
        visible,
        HEAD_SMALL,
    )
    attended_small, part_latent, paired_early, paired_late, lowered_parts = (
        lax.optimization_barrier(
            (attended_small, part_latent, paired_early, paired_late, lowered_parts)
        )
    )
    paired_near = across(paired_plans, paired_early)
    lowered_plans, lowered_early, lowered_late = widen(lowered_parts)
    attended_large = attend(
        nope_large,
        turned_large,
        lift(key_up_large),
        lift(value_up_large),
        turned_key,
        visible,
        HEAD_LARGE,
    )
    attended_large, paired_near, paired_late = lax.optimization_barrier(
        (attended_large, paired_near, paired_late)
    )
    paired_far = across(paired_plans, paired_late)
    share_mixed = jnp.dot(
        attended_small, out_small, preferred_element_type=jnp.float32
    ) + jnp.dot(attended_large, out_large, preferred_element_type=jnp.float32)
    share_mixed = share_mixed.reshape(tp_count, own_rows, share_mixed.shape[1])
    mixed = lax.dynamic_index_in_dim(share_mixed, tp_index, 0, False)
    for step in range(1, tp_count):
        sent = lax.dynamic_index_in_dim(share_mixed, tp_index ^ step, 0, False)
        mixed = mixed + tp_swap(sent.astype(jnp.bfloat16), step).astype(jnp.float32)
    mixed = mixed.astype(jnp.bfloat16)
    stream = (residual.astype(jnp.float32) + mixed.astype(jnp.float32)).astype(jnp.bfloat16)
    as_float = stream.astype(jnp.float32)
    normed = as_float * lax.rsqrt(jnp.mean(as_float * as_float, axis=-1, keepdims=True) + norm_eps)
    normed = (normed * norm_gain.astype(jnp.float32)[None, :]).astype(jnp.bfloat16)

    piece = normed
    for number, bit in enumerate(reversed(bits_below(far))):
        if number == 1:
            piece, paired_far, lowered_early, lowered_late = lax.optimization_barrier(
                (piece, paired_far, lowered_early, lowered_late)
            )
        piece = jnp.concatenate([piece, far_swap(piece, bit)], axis=0)
    lowered_near = across(lowered_plans, lowered_early)
    lowered_far = across(lowered_plans, lowered_late)

    def in_order(*kinds):
        return [block for group in zip(*kinds) for block in group]

    paired_weights = in_order(paired_early, paired_late, paired_near, paired_far)
    lowered_weights = in_order(lowered_early, lowered_late, lowered_near, lowered_far)
    piece = jnp.concatenate([tp_swap(piece, step) for step in range(tp_count)], axis=0)
    columns = by_distance([piece[:, z * depth : (z + 1) * depth] for z in range(sp_count)])
    both = None
    for order, weight in zip(orders_of(paired_plans), paired_weights):
        rows = jnp.concatenate([columns[place] for place in order], axis=1)
        product = jnp.dot(rows, weight, preferred_element_type=jnp.float32)
        both = product if both is None else both + product
    hidden = (jax.nn.silu(both[:, :share]) * both[:, share:]).astype(jnp.bfloat16)
    blocks = [None] * sp_count
    for order, weight in zip(orders_of(lowered_plans), lowered_weights):
        product = lax.dot_general(
            hidden, weight, (((1,), (1,)), ((), ())), preferred_element_type=jnp.float32
        ).astype(jnp.bfloat16)
        for number, place in enumerate(order):
            blocks[place] = product[:, number * depth : (number + 1) * depth]
    partial = jnp.concatenate(by_distance(blocks), axis=1)
    over_tp = partial.reshape(tp_count, far * own_rows, partial.shape[1])
    summed = over_tp[0].astype(jnp.float32)
    for step in range(1, tp_count):
        summed = summed + tp_swap(over_tp[step], step).astype(jnp.float32)
    for bit in bits_below(far):
        half = summed.shape[0] // 2
        sent = far_swap(summed[half:].astype(jnp.bfloat16), bit)
        summed = summed[:half] + sent.astype(jnp.float32)
    channel = summed
    channel = channel.astype(jnp.bfloat16)
    return (as_float + 0.5 * channel.astype(jnp.float32)).astype(jnp.bfloat16)


def solution(mesh):
    placed = (
        P(("sp", "tp"), None),
        P("sp", "tp"),
        P("sp", "tp"),
        P("sp", None),
        P("sp", None),
        P(None, "tp"),
        P(None, "tp"),
        P(None, "tp"),
        P(None, "tp"),
        P("tp", None),
        P("tp", None),
        P(),
        P("sp", "tp"),
        P("sp", "tp"),
        P("sp", "tp"),
    )
    return jax.shard_map(
        shards, mesh=mesh, in_specs=placed, out_specs=P(("sp", "tp"), None), check_vma=False
    )
```
